128 devices in a mesh: grp: 4 (over y, x), ep: 32 (over z, core).
Axes of the slice: x: 2, y: 2, z: 16, core: 2. Of those that a mesh axis runs over, the one named last changes fastest.
The devices are a block of a 8x8x16 slice.
Arguments:
- tokens: bfloat16 [2048, 2048], P(('grp', 'ep')), parts along dimension 0, may hold values from -6 to 6
- norm_gain: bfloat16 [2048], replicated, may hold values from 0.099609375 to 1.8984375
- query_weight: bfloat16 [2048, 1024], P(None, 'ep'), may hold values from -0.125 to 0.125
- key_weight: bfloat16 [2048, 256], replicated, may hold values from -0.25 to 0.25
- value_weight: bfloat16 [2048, 256], replicated, may hold values from -0.125 to 0.125
- out_weight: bfloat16 [1024, 2048], P(None, 'ep'), may hold values from -0.1875 to 0.1875
- head_gain: bfloat16 [128], replicated, may hold values from 0.099609375 to 1.8984375
- lambdas: float32 [8], replicated, may hold values from 0.3 to 0.8
- cache_keys: bfloat16 [2048, 1024, 2, 128], P(('grp', 'ep')), parts along dimension 0, may hold values from -1000 to 1000
- cache_values: bfloat16 [2048, 1024, 2, 128], P(('grp', 'ep')), parts along dimension 0, may hold values from -6 to 6
- lengths: int32 [2048], P(('grp', 'ep')), parts along dimension 0, may hold values from 64 to 1024
- moe_gain: bfloat16 [2048], replicated, may hold values from 0.099609375 to 1.8984375
- gate_weight: bfloat16 [32, 2048, 1024], P('ep'), may hold values from -0.375 to 0.375
- up_weight: bfloat16 [32, 2048, 1024], P('ep'), may hold values from -0.375 to 0.375
- down_weight: bfloat16 [32, 1024, 2048], P('ep'), may hold values from -0.02734375 to 0.02734375
- routes: int32 [2048, 4], P(('grp', 'ep')), parts along dimension 0, may hold values from 0 to 31, all different within a row; in each aligned block of 16 rows (0 to 15, 16 to 31, ...) at most 4 rows name the same one
- route_weights: float32 [2048, 4], P(('grp', 'ep')), parts along dimension 0, may hold values from 0.2 to 1
Outputs:
- mixed: bfloat16 [2048, 2048], P(('grp', 'ep')), parts along dimension 0
The draws below stay inside these ranges and needn't reach their ends.
There are 4 independent parts, one for each index of `grp`. The reference program is written for one: setup_inputs(seed, part) draws one part's arguments, and reference() takes and returns one part's arrays. A program takes and returns all parts, laid end to end along the dimension named above; an argument that names none is the same for every part. Nothing has to cross between parts.
Inputs may be any that keep to these rules, and one draw needn't show every extreme that they name: `routes`: a token's 4 experts differ; the tokens of one device name each expert at most 4 times, and in every draw some expert is named exactly 4 times by one device's tokens.
All inputs are finite; a program needn't handle non-finite values.
Results may differ from the reference program's by a relative error of at most 0.034.
Values may be sent and summed in bfloat16 or wider, within the bound.
A program may use at most 128 MiB of HBM per device.

```python
import math
import jax
import jax.numpy as jnp
import numpy as np
from jax import lax

D = 2048
HEADS = 8
KV_HEADS = 2
DH = 64
VAL = 128
FF = 1024
TOPK = 4
SEQ_DEV = 16
CTX = 1024
EXPERTS = 32
CAP = 4
SEQS = 512
N_EP = 32


def draw_cache_keys(key, part):
    shape = (SEQS, CTX, KV_HEADS, 2 * DH)
    base = jax.random.normal(key, shape, jnp.float32) * 1.75
    return base.astype(jnp.bfloat16)


def plant(entries, stream_key, smallest, largest):
    longest = entries.shape.index(max(entries.shape))
    spots = []
    for shift in (0, 1):
        where = [jax.random.randint(jax.random.fold_in(stream_key, axis), (), 0, length) for axis, length in enumerate(entries.shape)]
        where[longest] = (where[longest] + shift) % entries.shape[longest]
        spots.append(tuple(where))
    return entries.at[spots[0]].set(smallest).at[spots[1]].set(largest)


def shard_levels(key, extent, cuts, low, top_value):
    def one(dim, parts):
        heights = jax.random.uniform(jax.random.fold_in(jax.random.fold_in(key, 6), dim), (parts,), jnp.float32, low / len(cuts), top_value / len(cuts))
        return jnp.repeat(jnp.exp(heights), extent[dim] // parts).reshape((-1,) + (1,) * (len(extent) - dim - 1))

    level = one(*cuts[0])
    for cut in cuts[1:]:
        level = level * one(*cut)
    return level


def shared_out(rng, own, number, rows, amount, top, reach, skew):
    ranking = jax.random.permutation(rng, amount)
    packed, common = portions_of(amount, rows * top, reach, skew, True), portions_of(amount, rows * top, reach, skew, False)
    places = jnp.arange(amount)

    def named(tallies, offset_by):
        used = int((tallies > 0).sum())
        fixed = max(1, used // 4)
        moved = fixed + (places - fixed + offset_by * (used - fixed)) % max(1, amount - fixed)
        return jnp.zeros((amount,), jnp.int32).at[ranking[jnp.where(places < fixed, places, moved)]].set(jnp.asarray(tallies, jnp.int32))

    tallies = jnp.where(number % 4 == 0, named(packed, number // 4), named(common, number - number // 4 - 1))
    mixed = jax.random.permutation(jax.random.fold_in(own, 3), amount)
    donor, taker = mixed[0:amount // 2 * 2:2], mixed[1:amount // 2 * 2:2]
    room = jnp.minimum(tallies[donor] - 1, reach - tallies[taker]) // 2
    room = jnp.where((donor == ranking[0]) | (taker == ranking[0]) | (tallies[taker] == 0), 0, jnp.maximum(room, 0))
    moved = jax.random.randint(jax.random.fold_in(own, 4), (amount // 2,), 0, 1 << 20) % (room + 1)
    tallies = tallies.at[donor].add(-moved).at[taker].add(moved)
    members = jnp.searchsorted(jnp.cumsum(tallies), jnp.arange(rows * top), side="right").astype(jnp.int32)
    listing = members.reshape(top, rows).T
    listing = listing[jax.random.permutation(jax.random.fold_in(own, 1), rows)]
    offset_by = jax.random.randint(jax.random.fold_in(own, 2), (rows, 1), 0, top)
    return jnp.take_along_axis(listing, (jnp.arange(top)[None, :] + offset_by) % top, axis=1)


def portions_of(amount, total, bound, lean, full):
    portions = [(1 << 20) // math.isqrt(standing ** lean) + 1 for standing in range(1, amount + 1)]
    largest = bound if full else min(bound, max(-(-total // amount), total * portions[0] // sum(portions)))
    least = 1 if total - largest >= amount - 1 else 0
    counts, surplus = [largest] + [least] * (amount - 1), total - largest - least * (amount - 1)
    while surplus > 0:
        candidates = [i for i in range(1, amount) if counts[i] < largest] or [i for i in range(1, amount) if counts[i] < bound]
        whole, budget = sum([portions[i] for i in candidates]), surplus
        for i in candidates:
            more = min(bound - counts[i], max(1, budget * portions[i] // whole), surplus)
            counts[i] = counts[i] + more
            surplus = surplus - more
    return np.array(counts)


def centred(rng, shape, scale, most, cuts=(), held_as=jnp.bfloat16):
    drawn = scale * jax.random.normal(rng, shape, jnp.float32)
    if cuts:
        drawn = drawn * shard_levels(rng, shape, cuts, -0.22, 0.18)
    return jnp.clip(drawn, -most, most).astype(held_as)


def setup_inputs(seed: int = 0, part: int = 0) -> dict:
    arg_keys = jax.random.split(jax.random.key(seed), 18)
    part_keys = jax.random.split(jax.random.fold_in(arg_keys[17], part), 18)
    tokens = centred(part_keys[0], (SEQS, D), 1.0, 6.0, ((0, 32),))
    norm_gain = jnp.clip(1.0 + 0.18 * jax.random.normal(arg_keys[1], (D,), jnp.float32), 0.099609375, 1.8984375).astype(jnp.bfloat16)
    query_weight = centred(arg_keys[2], (D, 2 * HEADS * DH), D ** -0.5, 0.125, ((1, 32),))
    key_weight = centred(arg_keys[3], (D, 2 * KV_HEADS * DH), (D // 4) ** -0.5, 0.25)
    value_weight = centred(arg_keys[4], (D, KV_HEADS * VAL), D ** -0.5, 0.125)
    out_weight = centred(arg_keys[5], (HEADS * VAL, D), (HEADS * VAL) ** -0.5, 0.1875, ((1, 32),))
    head_gain = jnp.clip(1.0 + 0.18 * jax.random.normal(arg_keys[6], (VAL,), jnp.float32), 0.099609375, 1.8984375).astype(jnp.bfloat16)
    lambdas = jnp.clip(jax.random.uniform(arg_keys[7], (HEADS,), jnp.float32, 0.3, 0.8), 0.3, 0.8)
    cache_keys = draw_cache_keys(jax.random.fold_in(jax.random.fold_in(arg_keys[17], part), 71), part)
    cache_values = centred(part_keys[9], (SEQS, CTX, KV_HEADS, VAL), 1.0, 6.0, ((0, 32),))
    lengths = plant(jax.random.randint(part_keys[10], (SEQS,), CTX // 16, CTX + 1), jax.random.fold_in(part_keys[10], 1), CTX // 16, CTX).astype(jnp.int32)
    moe_gain = jnp.clip(1.0 + 0.18 * jax.random.normal(arg_keys[11], (D,), jnp.float32), 0.099609375, 1.8984375).astype(jnp.bfloat16)
    gate_weight = centred(arg_keys[12], (EXPERTS, D, FF), (D // 9) ** -0.5, 0.375, ((0, 32),))
    up_weight = centred(arg_keys[13], (EXPERTS, D, FF), (D // 9) ** -0.5, 0.375, ((0, 32),))
    down_weight = centred(arg_keys[14], (EXPERTS, FF, D), (FF * 48) ** -0.5, 0.02734375, ((0, 32),))
    routes_keys = jax.random.split(jax.random.fold_in(part_keys[15], 1), SEQS // SEQ_DEV)
    routes_turns = jax.random.permutation(jax.random.fold_in(part_keys[15], 3), SEQS // SEQ_DEV)
    routes = jax.vmap(lambda own, number: shared_out(jax.random.fold_in(part_keys[15], 2), own, number, SEQ_DEV, EXPERTS, TOPK, CAP, 2))(routes_keys, routes_turns).reshape((SEQS, TOPK))
    route_weights = jnp.clip(0.2 + 0.8 * jax.random.uniform(part_keys[16], (SEQS, TOPK), jnp.float32) ** shard_levels(part_keys[16], (SEQS, TOPK), ((0, 32),), -0.2, 0.2), 0.2, 1.0)
    return dict(tokens=tokens, norm_gain=norm_gain, query_weight=query_weight, key_weight=key_weight, value_weight=value_weight, out_weight=out_weight, head_gain=head_gain, lambdas=lambdas, cache_keys=cache_keys, cache_values=cache_values, lengths=lengths, moe_gain=moe_gain, gate_weight=gate_weight, up_weight=up_weight, down_weight=down_weight, routes=routes, route_weights=route_weights)


epsilon = 1e-06
masked_score = -1e+30
clamp_limit = 7.0
swish_alpha = 1.702

def rms_scaled(values, gain):
    floats = values.astype(jnp.float32)
    return floats * lax.rsqrt(lax.optimization_barrier(jnp.mean(floats * floats, axis=-1, keepdims=True)) + epsilon) * gain.astype(jnp.float32)

def attention(queries, new_keys, new_values, cache_keys, cache_values, lengths, lambdas, head_gain):
    count = queries.shape[0]
    ctx_len = cache_keys.shape[1]
    kv_count = cache_keys.shape[2]
    head_dim = cache_keys.shape[3] // 2
    heads = lambdas.shape[0]
    group = heads // kv_count
    val_dim = cache_values.shape[3]
    query_grid = queries.reshape(count, kv_count, group, 2, head_dim).astype(jnp.float32)
    key_grid = cache_keys.reshape(count, ctx_len, kv_count, 2, head_dim).astype(jnp.float32)
    own_keys = new_keys.reshape(count, kv_count, 2, head_dim).astype(jnp.float32)
    inv_scale = head_dim ** (-0.5)
    scores = jnp.einsum('bkgcd,bjkcd->bkgcj', query_grid, key_grid) * inv_scale
    own_score = jnp.einsum('bkgcd,bkcd->bkgc', query_grid, own_keys) * inv_scale
    visible = jnp.arange(ctx_len, dtype=jnp.int32)[None, :] < lengths[:, None]
    scores = jnp.where(visible[:, None, None, None, :], scores, masked_score)
    highest = jnp.maximum(lax.optimization_barrier(jnp.max(scores, axis=-1)), own_score)
    expd = jnp.exp(scores - highest[..., None])
    own_exp = jnp.exp(own_score - highest)
    denominator = lax.optimization_barrier(jnp.sum(expd, axis=-1)) + own_exp
    probs = expd / denominator[..., None]
    own_prob = own_exp / denominator
    lambda_grid = lambdas.reshape(kv_count, group)[None, :, :]
    weights = (probs[:, :, :, 0] - lambda_grid[..., None] * probs[:, :, :, 1]).astype(jnp.bfloat16)
    own_weight = (own_prob[..., 0] - lambda_grid * own_prob[..., 1]).astype(jnp.bfloat16)
    attended = jnp.einsum('bkgj,bjkv->bkgv', weights.astype(jnp.float32), cache_values.astype(jnp.float32))
    own_vals = new_values.reshape(count, kv_count, val_dim).astype(jnp.float32)
    attended = attended + own_weight.astype(jnp.float32)[..., None] * own_vals[:, :, None, :]
    return rms_scaled(attended, head_gain).reshape(count, heads * val_dim).astype(jnp.bfloat16)

def expert_mlp(inputs, gate_w, up_w, down_w):
    gate = jnp.dot(inputs, gate_w, preferred_element_type=jnp.float32)
    upper = jnp.dot(inputs, up_w, preferred_element_type=jnp.float32)
    gate = jnp.minimum(gate, clamp_limit)
    upper = jnp.clip(upper, -clamp_limit, clamp_limit)
    act = ((upper + 1.0) * gate * jax.nn.sigmoid(swish_alpha * gate)).astype(jnp.bfloat16)
    return jnp.dot(act, down_w, preferred_element_type=jnp.float32).astype(jnp.bfloat16)

def reference(tokens, norm_gain, query_weight, key_weight, value_weight, out_weight, head_gain, lambdas, cache_keys, cache_values, lengths, moe_gain, gate_weight, up_weight, down_weight, routes, route_weights):
    count = tokens.shape[0]
    width = tokens.shape[1]
    normed = rms_scaled(tokens, norm_gain).astype(jnp.bfloat16)
    queries = jnp.dot(normed, query_weight, preferred_element_type=jnp.float32).astype(jnp.bfloat16)
    new_keys = jnp.dot(normed, key_weight, preferred_element_type=jnp.float32).astype(jnp.bfloat16)
    new_values = jnp.dot(normed, value_weight, preferred_element_type=jnp.float32).astype(jnp.bfloat16)
    head_out = attention(queries, new_keys, new_values, cache_keys, cache_values, lengths, lambdas, head_gain)
    attn_out = jnp.dot(head_out, out_weight, preferred_element_type=jnp.float32).astype(jnp.bfloat16)
    residual = (tokens.astype(jnp.float32) + attn_out.astype(jnp.float32)).astype(jnp.bfloat16)
    moe_in = rms_scaled(residual, moe_gain).astype(jnp.bfloat16)
    onehot = (routes.reshape(N_EP, SEQ_DEV * TOPK)[:, :, None] == jnp.arange(EXPERTS, dtype=jnp.int32)[None, None, :]).astype(jnp.int32)
    earlier = jnp.cumsum(onehot, axis=1) - onehot
    ranks = lax.optimization_barrier(jnp.sum(earlier * onehot, axis=2)).reshape(count, TOPK)
    block_of = jnp.broadcast_to((jnp.arange(count, dtype=jnp.int32) // SEQ_DEV)[:, None], (count, TOPK))
    slot_index = (routes * (N_EP * CAP) + block_of * CAP + ranks).astype(jnp.int32).reshape(-1)
    copies = jnp.broadcast_to(moe_in[:, None, :], (count, TOPK, width)).reshape(-1, width)
    buffer = jnp.zeros((EXPERTS * N_EP * CAP, width), jnp.bfloat16).at[slot_index].set(copies)
    buffer = buffer.reshape(EXPERTS, N_EP * CAP, width)
    results = lax.map(lambda group: expert_mlp(group[0], group[1], group[2], group[3]), (buffer, gate_weight, up_weight, down_weight))
    picked = results.reshape(-1, width)[slot_index].reshape(count, TOPK, width)
    moe_sum = lax.optimization_barrier(jnp.sum(route_weights[:, :, None] * picked.astype(jnp.float32), axis=1))
    return (residual.astype(jnp.float32) + moe_sum).astype(jnp.bfloat16)
```

```python
import functools

import jax
import jax.numpy as jnp
from jax import lax
from jax.experimental import pallas as pl
from jax.experimental.pallas import tpu as pltpu
from jax.sharding import PartitionSpec as P

EPS = 1e-06
NEG = -1e30
LIMIT = 7.0
ALPHA = 1.702
F32 = jnp.float32
BF16 = jnp.bfloat16
MESH = pl.DeviceIdType.MESH
META = 128
PIECES = 2
WO_PIECES = 4
CACHE_STEPS = 4


def iota(shape, dim):
    return lax.broadcasted_iota(jnp.int32, shape, dim)


def mask(cond):
    return jnp.where(cond, 1.0, 0.0).astype(F32)


def dot(a, b, dims=(((1,), (0,)), ((), ()))):
    return lax.dot_general(a, b, dims, preferred_element_type=F32)


def scaled(x, gain):
    return x * lax.rsqrt(jnp.mean(x * x, axis=-1, keepdims=True) + EPS) * gain


def kernel(
    nz, kv, lam_ref, len_ref, tok_ref, ng_ref, hg_ref, mg_ref, routes_ref, rw_ref,
    wq_hbm, wk_hbm, wv_hbm, wo_hbm, keys_hbm, vals_hbm, gate_hbm, up_hbm, down_hbm,
    out_ref,
    kbuf, vbuf, gbuf, ubuf, dbuf, wqb, wqp, wq128, wkb, wvb, wob,
    xg, wog, qs, qr, qall, owns, vown, hof, attn, res, mx, xc, xe, ye, yo, yr, act,
    rf, rin_r, rin_l, st_f, st_w,
    lsem, cache_sem, pair_send, pair_recv,
    x_sr, x_sl, x_rc, wo_sr, wo_sl, wo_rc, wop_s, wop_r, q_s, q_r,
    m_sr, m_sl, m_rc, r_sr, r_sl, r_rr, r_rl,
):
    rows, width = tok_ref.shape
    heads = 2 * nz * 64 // 2 // 64 // 2
    group = heads // kv
    ctx2 = kbuf.shape[1]
    half = nz // 2
    kp = xg.shape[0]
    pw = width // kp
    kw = wo_sr.shape[1]
    me = lax.axis_index("ep")
    z = lax.div(me, 2)
    c = lax.rem(me, 2)

    def wrap(v):
        return lax.rem(v + 2 * nz, nz)

    def dev(zz, cc):
        return {"ep": zz * 2 + cc}

    right = dev(wrap(z + 1), c)
    left = dev(wrap(z - 1), c)
    partner = dev(z, 1 - c)
    sent = []

    def send(src, dst, ssem, rsem, to):
        cp = pltpu.make_async_remote_copy(
            src_ref=src, dst_ref=dst, send_sem=ssem, recv_sem=rsem, device_id=to, device_id_type=MESH
        )
        cp.start()
        sent.append(cp)

    def arrived(dst, rsem, ssem):
        pltpu.make_async_remote_copy(
            src_ref=dst, dst_ref=dst, send_sem=ssem, recv_sem=rsem, device_id=right, device_id_type=MESH
        ).wait_recv()

    loads = {}

    def load(name, src, dst, sem):
        cp = pltpu.make_async_copy(src, dst, sem)
        cp.start()
        loads[name] = cp

    load("wq", wq_hbm, wqb, lsem.at[0])
    load("wo", wo_hbm, wob, lsem.at[1])
    load("wk", wk_hbm, wkb, lsem.at[2])
    load("wv", wv_hbm, wvb, lsem.at[3])
    steps = cache_sem.shape[1]
    per = rows // steps
    for i in range(steps):
        part = pl.ds(i * per, per)
        load(("k", i), keys_hbm.at[part], kbuf.at[part], cache_sem.at[0, i])
        load(("v", i), vals_hbm.at[part], vbuf.at[part], cache_sem.at[1, i])
    load("gate", gate_hbm.at[0], gbuf, lsem.at[4])
    load("up", up_hbm.at[0], ubuf, lsem.at[5])
    load("down", down_hbm.at[0], dbuf, lsem.at[6])

    barrier = pltpu.get_barrier_semaphore()
    for i in range(1, nz):
        pl.semaphore_signal(barrier, inc=1, device_id=dev(wrap(z + i), c), device_id_type=MESH)
    pl.semaphore_signal(barrier, inc=1, device_id=partner, device_id_type=MESH)

    tokens = tok_ref[...].astype(F32)
    normed = scaled(tokens, ng_ref[...].astype(F32)).astype(BF16)
    weight = rw_ref[...]
    topk = weight.shape[1]
    hi = weight.astype(BF16).astype(F32)
    lo = weight - hi
    lane = iota((rows, META), 1)
    meta = jnp.zeros((rows, META), F32)
    routes = routes_ref[...].astype(F32)
    for k in range(topk):
        meta = jnp.where(lane == k, routes[:, k : k + 1], meta)
        meta = jnp.where(lane == topk + k, hi[:, k : k + 1], meta)
        meta = jnp.where(lane == 2 * topk + k, lo[:, k : k + 1], meta)
    for p in range(kp):
        xg[p, 0, :, 0:pw] = normed[:, p * pw : (p + 1) * pw]
        xg[p, 0, :, pw : pw + META] = meta.astype(BF16)

    pl.semaphore_wait(barrier, nz)

    def hop(buf, h, s_r, s_l, r_c):
        for p in range(kp):
            if h >= 1:
                arrived(buf.at[p, h], r_c.at[p, h], s_r.at[p, h - 1])
            if h < half:
                send(buf.at[p, h], buf.at[p, h + 1], s_r.at[p, h], r_c.at[p, h + 1], right)
            if 1 <= h < half:
                arrived(buf.at[p, nz - h], r_c.at[p, nz - h], s_l.at[p, h - 1])
            if h < half - 1:
                back = (nz - h) % nz
                send(buf.at[p, back], buf.at[p, nz - h - 1], s_l.at[p, h], r_c.at[p, nz - h - 1], left)

    wrows = wog.shape[2] // kw

    def wo_task(h, p):
        part = pl.ds(p * wrows, wrows)
        a, b = wrap(z - h), wrap(z + h)
        if h >= 1:
            arrived(wog.at[c, a, part], wo_rc.at[h, p], wo_sr.at[h - 1, p])
        if h < half:
            ref = wog.at[c, a, part]
            send(ref, ref, wo_sr.at[h, p], wo_rc.at[h + 1, p], right)
        if 1 <= h < half:
            arrived(wog.at[c, b, part], wo_rc.at[nz - h, p], wo_sl.at[h - 1, p])
        if h < half - 1:
            ref = wog.at[c, b, part]
            send(ref, ref, wo_sl.at[h, p], wo_rc.at[nz - h - 1, p], left)
        if p == kw - 1:
            send(wog.at[c, a], wog.at[c, a], wop_s.at[h], wop_r.at[h], partner)
            if 1 <= h < half:
                send(wog.at[c, b], wog.at[c, b], wop_s.at[nz - h], wop_r.at[nz - h], partner)

    wo_tasks = [(h, p) for h in range(half + 1) for p in range(kw)]
    done = [0]

    def wo_run(n):
        for h, p in wo_tasks[done[0] : done[0] + n]:
            wo_task(h, p)
        done[0] += n

    def place(off):
        n = wqb.shape[1]
        return mask((iota((n, 128), 1) & 63) == iota((n, 128), 0) + off).astype(BF16)

    hop(xg, 0, x_sr, x_sl, x_rc)
    loads["wq"].wait()
    send(wqb, wqp, pair_send.at[0], pair_recv.at[0], partner)
    loads["wo"].wait()
    kd = wob.shape[0] // 2
    e0 = mask(iota((64, 128), 1) == iota((64, 128), 0)).astype(BF16)
    e1 = mask(iota((64, 128), 1) == iota((64, 128), 0) + 64).astype(BF16)
    wog[c, z] = (dot(wob[0:kd, :], e0) + dot(wob[kd : 2 * kd, :], e1)).astype(BF16)
    wo_run(1)

    nq = wqb.shape[1]
    own_q = dot(wqb[...], place(nq * c))
    arrived(wqp, pair_recv.at[0], pair_send.at[0])
    wq128[...] = (own_q + dot(wqp[...], place(nq * (1 - c)))).astype(BF16)

    lane8 = iota((rows // 2, 128), 1)
    first = lane8 < 64
    odd = lax.rem(z, 2)
    upper = jnp.where(first, 0, 1) == odd

    def query_block(r):
        q = dot(xg[0, r, :, 0:pw], wq128[0:pw, :])
        for p in range(1, kp):
            q = q + dot(xg[p, r, :, 0:pw], wq128[p * pw : (p + 1) * pw, :])
        return jnp.where(upper, q[0 : rows // 2], q[rows // 2 : rows]).astype(BF16)

    def query_send(r):
        qs[r] = query_block(r)
        origin = wrap(z - r)
        send(qs.at[r], qr.at[z], q_s.at[r], q_r.at[z], dev(origin, c))

    hop(xg, 1, x_sr, x_sl, x_rc)
    wo_run(1)
    qr[z] = query_block(0)
    loads["wk"].wait()
    loads["wv"].wait()
    new_keys = dot(normed, wkb[...]).astype(BF16)
    new_vals = dot(normed, wvb[...]).astype(BF16)
    query_send(1)
    query_send(nz - 1)
    for h in range(2, half + 1):
        hop(xg, h, x_sr, x_sl, x_rc)
        if h < half:
            wo_run(1)
        query_send(h)
        if h < half:
            query_send(nz - h)

    nrow = rows * nz
    def rep(n, per_tok, nh, x):
        i0, i1 = iota((n, kv * rows), 0), iota((n, kv * rows), 1)
        tok_i, head_i = lax.div(i0, per_tok), lax.rem(i0, nh)
        sel = (lax.rem(i1, rows) == tok_i) & (lax.div(i1, rows) == lax.div(head_i, group))
        stacked = jnp.concatenate([x[:, i * 128 : (i + 1) * 128] for i in range(kv)], axis=0)
        return dot(mask(sel).astype(BF16), stacked)

    key_rows = rep(nrow, nz, heads, new_keys)
    vown[...] = rep(rows * heads, heads, heads, new_vals).reshape(rows, heads, 128)

    ntok = nz * rows
    mt = xg[0, :, :, pw : pw + META].reshape(ntok, META).astype(F32)
    rt, wt = mt[:, 0:topk], mt[:, topk : 2 * topk] + mt[:, 2 * topk : 3 * topk]
    cap = st_f.shape[1] // (2 * nz)

    def hit(e):
        is_e = mask(rt == e.astype(F32))
        return jnp.sum(is_e, axis=1, keepdims=True), jnp.sum(is_e * wt, axis=1, keepdims=True)

    h0, w0 = hit(me)
    h1, w1 = hit(2 * z + 1 - c)
    ns = st_f.shape[1]
    sl = iota((ntok, ns), 1)
    hb = jnp.where(sl < ns // 2, h0, h1)
    wb = jnp.where(sl < ns // 2, w0, w1)
    t0, t1 = iota((ntok, ntok), 0), iota((ntok, ntok), 1)
    before = mask((lax.div(t0, rows) == lax.div(t1, rows)) & (t1 < t0)).astype(BF16)
    rank = dot(before, hb.astype(BF16))
    slot = (cap * lax.div(iota((ntok, ns), 0), rows)).astype(F32) + rank
    sel = jnp.where((hb > 0.5) & (slot == lax.rem(sl, ns // 2).astype(F32)), 1.0, 0.0)
    st_f[...] = sel
    sw = sel * wb
    sw_hi = sw.astype(BF16)
    st_w[0] = sw_hi
    st_w[1] = (sw - sw_hi.astype(F32)).astype(BF16)

    wo_run(kw)
    for r in range(1, nz):
        src = wrap(z - r)
        arrived(qr.at[src], q_r.at[src], q_s.at[r])
    qf = qr[...].reshape(nz * rows // 2, 128)
    i0 = iota((nz * rows // 2, 128), 0)
    mine = lax.rem(lax.div(i0, rows // 2), 2) == lax.div(iota((nz * rows // 2, 128), 1), 64)
    qf32 = qf.astype(F32)
    q_lo = jnp.where(mine, qf32, 0.0).astype(BF16)
    q_hi = jnp.where(mine, pltpu.roll(qf32, 64, 1), 0.0).astype(BF16)
    qcat = jnp.concatenate([q_lo, q_hi], axis=0)
    o = iota((nrow, nrow), 0)
    ot, oj = lax.div(o, nz), lax.rem(o, nz)
    src_z = 2 * lax.rem(oj, heads) + lax.div(oj, heads)
    hr = rows // 2
    src_row = lax.div(ot, hr) * (nz * hr) + src_z * hr + lax.rem(ot, hr)
    qperm = dot(mask(src_row == iota((nrow, nrow), 1)).astype(BF16), qcat)
    qall[...] = qperm.astype(BF16).reshape(rows, nz, 128)
    scale = 64 ** (-0.5)
    own_score = jnp.sum(qperm * key_rows, axis=1, keepdims=True) * scale
    owns[...] = jnp.broadcast_to(own_score, (nrow, 128)).reshape(rows, nz, 128)

    lam = jnp.zeros((heads, 1), F32)
    for i in range(heads):
        lam = jnp.where(iota((heads, 1), 0) == i, lam_ref[i], lam)
    hgain = hg_ref[...].astype(F32)
    col = iota((nz, ctx2), 1)
    head_of = lax.rem(iota((nz, ctx2), 0), heads)
    kv_ok = lax.rem(col, kv) == lax.div(head_of, group)
    pos = jnp.where(kv_ok, lax.div(col, kv), 1 << 30)

    def attend(t):
        s = dot(qall[t], kbuf[t], (((1,), (1,)), ((), ()))) * scale
        s = jnp.where(pos < len_ref[t], s, NEG)
        own = owns[t][:, 0:1]
        top = jnp.maximum(jnp.max(s, axis=1, keepdims=True), own)
        e = jnp.exp(s - top)
        eo = jnp.exp(own - top)
        den = jnp.sum(e, axis=1, keepdims=True) + eo
        inv = 1.0 / den
        w = (e[0:heads] * inv[0:heads] - (lam * inv[heads:nz]) * e[heads:nz]).astype(BF16)
        wo = (eo[0:heads] * inv[0:heads] - lam * (eo[heads:nz] * inv[heads:nz])).astype(BF16)
        a = dot(w, vbuf[t]) + wo.astype(F32) * vown[t]
        hof[t] = scaled(a, hgain).astype(BF16).astype(F32)

    for i in range(steps):
        wo_run(kw)
        loads[("k", i)].wait()
        loads[("v", i)].wait()

        def body(j, carry):
            attend(i * per + 2 * j)
            attend(i * per + 2 * j + 1)
            return carry

        lax.fori_loop(0, per // 2, body, 0)
    wo_run(len(wo_tasks) - done[0])
    for h in range(half + 1):
        arrived(wog.at[1 - c, wrap(z - h)], wop_r.at[h], wop_s.at[h])
        if 1 <= h < half:
            arrived(wog.at[1 - c, wrap(z + h)], wop_r.at[nz - h], wop_s.at[nz - h])

    hh = heads // 2
    ho = jnp.concatenate(
        [
            jnp.concatenate([hof[:, h, :] for h in range(s * hh, (s + 1) * hh)], axis=1)
            for s in range(2)
        ],
        axis=0,
    ).astype(BF16)
    lo64 = iota((rows, 128), 1) < 64

    def project(j, carry):
        p0 = dot(ho, wog[0, j])
        p1 = dot(ho, wog[1, j])
        direct = jnp.where(lo64, p0[0:rows], p1[rows : 2 * rows])
        turned = jnp.where(lo64, p1[0:rows], p0[rows : 2 * rows])
        attn[j] = direct + pltpu.roll(turned, 64, 1)
        return carry

    lax.fori_loop(0, nz, project, 0)
    total = jnp.zeros((rows, 1), F32)
    for j in range(nz):
        cols = slice(j * 128, (j + 1) * 128)
        v = tok_ref[:, cols].astype(F32) + attn[j].astype(BF16).astype(F32)
        v = v.astype(BF16).astype(F32)
        res[:, cols] = v
        total = total + jnp.sum(v * v, axis=1, keepdims=True)
    inv_rms = lax.rsqrt(total / width + EPS)
    for p in range(kp):
        cols = slice(p * pw, (p + 1) * pw)
        mx[p, 0] = (res[:, cols] * inv_rms * mg_ref[:, cols].astype(F32)).astype(BF16)

    for h in range(half + 1):
        hop(mx, h, m_sr, m_sl, m_rc)

    comp = st_f[...].T.astype(BF16)
    nhalf = ns // 2
    for p in range(kp):
        rows_p = dot(comp, mx[p].reshape(ntok, pw)).astype(BF16)
        xc[p] = rows_p[nhalf:ns]
        send(xc.at[p], xe.at[p, 1], pair_send.at[1 + p], pair_recv.at[1 + p], partner)
        xe[p, 0] = rows_p[0:nhalf]

    loads["gate"].wait()
    loads["up"].wait()
    for p in range(kp):
        arrived(xe.at[p, 1], pair_recv.at[1 + p], pair_send.at[1 + p])
    x = jnp.concatenate([xe[p].reshape(ns, pw) for p in range(kp)], axis=1)
    tile = 256

    def hidden(j, carry):
        cols = pl.ds(pl.multiple_of(j * tile, tile), tile)
        g = jnp.minimum(dot(x, gbuf[:, cols]), LIMIT)
        u = jnp.clip(dot(x, ubuf[:, cols]), -LIMIT, LIMIT)
        act[:, cols] = ((u + 1.0) * g / (1.0 + jnp.exp(-ALPHA * g))).astype(BF16)
        return carry

    lax.fori_loop(0, gbuf.shape[1] // tile, hidden, 0)
    loads["down"].wait()
    av = act[...]
    for p in range(kp):
        y = dot(av, dbuf[:, p * pw : (p + 1) * pw]).astype(BF16)
        ye[p] = y[nhalf:ns]
        send(ye.at[p], yr.at[p], pair_send.at[1 + kp + p], pair_recv.at[1 + kp + p], partner)
        yo[p] = y[0:nhalf]

    for p in range(kp):
        arrived(yr.at[p], pair_recv.at[1 + kp + p], pair_send.at[1 + kp + p])
        yy = jnp.concatenate([yo[p], yr[p]], axis=0)
        r = dot(st_w[0], yy) + dot(st_w[1], yy)
        rf[p] = r.astype(BF16).reshape(nz, rows, pw)
        send(rf.at[p, half], rin_r.at[p, 0], r_sr.at[p, 0], r_rr.at[p, 0], right)
        send(rf.at[p, half - 1], rin_l.at[p, 0], r_sl.at[p, 0], r_rl.at[p, 0], left)

    for t in range(half):
        for p in range(kp):
            arrived(rin_r.at[p, t], r_rr.at[p, t], r_sr.at[p, t])
            if t < half - 1:
                slot_r = half + 1 + t
                rf[p, slot_r] = (rf[p, slot_r].astype(F32) + rin_r[p, t].astype(F32)).astype(BF16)
                send(rf.at[p, slot_r], rin_r.at[p, t + 1], r_sr.at[p, t + 1], r_rr.at[p, t + 1], right)
            if t < half - 1:
                arrived(rin_l.at[p, t], r_rl.at[p, t], r_sl.at[p, t])
            if t < half - 2:
                slot_l = half - 2 - t
                rf[p, slot_l] = (rf[p, slot_l].astype(F32) + rin_l[p, t].astype(F32)).astype(BF16)
                send(rf.at[p, slot_l], rin_l.at[p, t + 1], r_sl.at[p, t + 1], r_rl.at[p, t + 1], left)
    for p in range(kp):
        cols = slice(p * pw, (p + 1) * pw)
        moe = rf[p, 0].astype(F32) + rin_r[p, half - 1].astype(F32) + rin_l[p, half - 2].astype(F32)
        out_ref[:, cols] = (res[:, cols] + moe).astype(BF16)

    for cp in sent:
        cp.wait_send()


def local(
    nz, tokens, norm_gain, query_weight, key_weight, value_weight, out_weight, head_gain, lambdas,
    cache_keys, cache_values, lengths, moe_gain, gate_weight, up_weight, down_weight, routes, route_weights,
):
    rows, width = tokens.shape
    ctx, kv, kd = cache_keys.shape[1:]
    ff = gate_weight.shape[2]
    keys = cache_keys.reshape(rows, ctx * kv, kd)
    vals = cache_values.reshape(rows, ctx * kv, kd)
    heads = lambdas.shape[0]
    half = nz // 2
    kp, kw = PIECES, WO_PIECES
    pw = width // kp
    ns = 2 * nz * 4
    kdim = out_weight.shape[0] // 2
    vmem, smem, anym = (pl.BlockSpec(memory_space=m) for m in (pltpu.VMEM, pltpu.SMEM, pl.ANY))
    dma = pltpu.SemaphoreType.DMA
    V = pltpu.VMEM
    scratch = [
        V(keys.shape, BF16), V(vals.shape, BF16),
        V((width, ff), BF16), V((width, ff), BF16), V((ff, width), BF16),
        V(query_weight.shape, BF16), V(query_weight.shape, BF16), V((width, 128), BF16),
        V(key_weight.shape, BF16), V(value_weight.shape, BF16), V(out_weight.shape, BF16),
        V((kp, nz, rows, pw + META), BF16),
        V((2, nz, kdim, 128), BF16),
        V((nz, rows // 2, 128), BF16), V((nz, rows // 2, 128), BF16),
        V((rows, nz, 128), BF16), V((rows, nz, 128), F32), V((rows, heads, 128), F32),
        V((rows, heads, 128), F32), V((nz, rows, 128), F32), V((rows, width), F32),
        V((kp, nz, rows, pw), BF16),
        V((kp, ns // 2, pw), BF16), V((kp, 2, ns // 2, pw), BF16),
        V((kp, ns // 2, pw), BF16), V((kp, ns // 2, pw), BF16), V((kp, ns // 2, pw), BF16),
        V((ns, ff), BF16),
        V((kp, nz, rows, pw), BF16), V((kp, half, rows, pw), BF16), V((kp, half, rows, pw), BF16),
        V((nz * rows, ns), F32), V((2, nz * rows, ns), BF16),
        dma((7,)), dma((2, CACHE_STEPS)), dma((1 + 2 * kp,)), dma((1 + 2 * kp,)),
        dma((kp, half)), dma((kp, half)), dma((kp, nz)),
        dma((half, kw)), dma((half, kw)), dma((nz, kw)),
        dma((nz,)), dma((nz,)), dma((nz,)), dma((nz,)),
        dma((kp, half)), dma((kp, half)), dma((kp, nz)),
        dma((kp, half)), dma((kp, half)), dma((kp, half)), dma((kp, half)),
    ]
    return pl.pallas_call(
        functools.partial(kernel, nz, kv),
        out_shape=jax.ShapeDtypeStruct((rows, width), BF16),
        in_specs=[smem, smem] + [vmem] * 6 + [anym] * 9,
        out_specs=vmem,
        scratch_shapes=scratch,
        compiler_params=pltpu.CompilerParams(
            collective_id=0, has_side_effects=True, vmem_limit_bytes=60 * 1024 * 1024
        ),
    )(
        lambdas, lengths, tokens, norm_gain.reshape(1, -1), head_gain.reshape(1, -1),
        moe_gain.reshape(1, -1), routes, route_weights,
        query_weight, key_weight, value_weight, out_weight, keys, vals,
        gate_weight, up_weight, down_weight,
    )


def solution(mesh):
    both = ("grp", "ep")
    return jax.shard_map(
        functools.partial(local, mesh.shape["ep"] // 2),
        mesh=mesh,
        in_specs=(
            P(both, None), P(), P(None, "ep"), P(), P(), P(None, "ep"), P(), P(),
            P(both, None, None, None), P(both, None, None, None), P(both), P(),
            P("ep", None, None), P("ep", None, None), P("ep", None, None),
            P(both, None), P(both, None),
        ),
        out_specs=P(both, None),
        check_vma=False,
    )
```
